32 devices in a mesh: grp: 2 (over x), ep: 16 (over z, y, core).
Axes of the slice: x: 2, y: 2, z: 4, core: 2. Of those that a mesh axis runs over, the one named last changes fastest.
Arguments:
- tokens: bfloat16 [32, 2048], P(('grp', 'ep')), parts along dimension 0, may hold values from -6 to 6
- cache_latent: bfloat16 [32, 3072, 512], P(('grp', 'ep')), parts along dimension 0, may hold values from -6 to 6
- cache_rope: bfloat16 [32, 32, 3072], P(('grp', 'ep')), parts along dimension 0, may hold values from -1000 to 1000
- lengths: int32 [32], P(('grp', 'ep')), parts along dimension 0, may hold values from 384 to 3072, as said below
- w_query: bfloat16 [2048, 1536], P('ep'), may hold values from -0.125 to 0.125
- w_latent: bfloat16 [2048, 512], P('ep'), may hold values from -0.125 to 0.125
- w_rope: bfloat16 [2048, 32], P('ep'), may hold values from -0.125 to 0.125
- w_absorb: bfloat16 [512, 1024], replicated, may hold values from -0.25 to 0.25
- w_value: bfloat16 [512, 1024], replicated, may hold values from -0.25 to 0.25
- w_output: bfloat16 [1024, 2048], P('ep'), may hold values from -0.1875 to 0.1875
- gain_attn: float32 [2048], replicated, may hold values from 0.1 to 1.9
- gain_latent: float32 [512], replicated, may hold values from 0.1 to 1.9
- gain_moe: float32 [2048], replicated, may hold values from 0.1 to 1.9
- routes: int32 [32, 2], P(('grp', 'ep')), parts along dimension 0, may hold values from 0 to 15, all different within a row; in each aligned block of 16 rows (0 to 15, 16 to 31, ...) at most 4 rows name the same one
- route_scores: float32 [32, 2], P(('grp', 'ep')), parts along dimension 0, may hold values from 0.2 to 1
- w_gate: bfloat16 [16, 2048, 512], P('ep'), may hold values from -0.125 to 0.125
- w_up: bfloat16 [16, 2048, 512], P('ep'), may hold values from -0.125 to 0.125
- w_down: bfloat16 [16, 512, 2048], P('ep'), may hold values from -0.25 to 0.25
Outputs:
- mixed: bfloat16 [32, 2048], P(('grp', 'ep')), parts along dimension 0
- new_latent: bfloat16 [32, 512], P(('grp', 'ep')), parts along dimension 0
- new_rope: bfloat16 [32, 32], P(('grp', 'ep')), parts along dimension 0
The draws below stay inside these ranges and needn't reach their ends.
There are 2 independent parts, one for each index of `grp`. The reference program is written for one: setup_inputs(seed, part) draws one part's arguments, and reference() takes and returns one part's arrays. A program takes and returns all parts, laid end to end along the dimension named above; an argument that names none is the same for every part. Nothing has to cross between parts.
Inputs may be any that keep to these rules, and one draw needn't show every extreme that they name: `routes`: each row names 2 different experts; over one part's 16 tokens no expert is named by more than 4 rows, a bound that some block reaches. `lengths`: some sequence has all 3072 positions filled.
All inputs are finite; a program needn't handle non-finite values.
Results may differ from the reference program's by a relative error of at most 0.013.
Values may be sent and summed in bfloat16 or wider, within the bound.
No kernel may reach another device: no remote copies, remote signals or barrier semaphores. Data moves between devices by JAX's collectives and lax.ppermute only.
A program may use at most 64 MiB of HBM per device.

```python
import math
import jax
import jax.numpy as jnp
import numpy as np
from jax import lax

D = 2048
HEADS = 16
NOPE = 64
ROPE = 32
VDIM = 64
LATENT = 512
FF = 512
TOPK = 2
CACHE = 3072
SEQS = 16
EXPERTS = 16
CAP = 4


def draw_cache_rope(key, part):
    k_base = jax.random.fold_in(jax.random.fold_in(key, 31), 0)
    base = jnp.clip(jax.random.normal(k_base, (SEQS, ROPE, CACHE), jnp.float32), -6.0, 6.0)
    return base.astype(jnp.bfloat16)


def draw_lengths(key, part):
    k_len, k_full = jax.random.split(jax.random.fold_in(key, 23))
    values = jax.random.randint(k_len, (SEQS,), CACHE // 8, CACHE + 1)
    chosen = jax.random.randint(k_full, (), 0, SEQS)
    values = jnp.where(jnp.arange(SEQS) == chosen, CACHE, values)
    return values.astype(jnp.int32)


def block_scale(own_key, extent, shards, low, top_value):
    def one(dim, shards_of):
        draws = jax.random.uniform(jax.random.fold_in(jax.random.fold_in(own_key, 6), dim), (shards_of,), jnp.float32, low / len(shards), top_value / len(shards))
        return jnp.repeat(jnp.exp(draws), extent[dim] // shards_of).reshape((-1,) + (1,) * (len(extent) - dim - 1))

    level = one(*shards[0])
    for cut in shards[1:]:
        level = level * one(*cut)
    return level


def assign_block(own_key, own, number, rows, number_of, top, most, lean):
    order = jax.random.permutation(own_key, number_of)
    crowded, ordinary = portions_of(number_of, rows * top, most, lean, True), portions_of(number_of, rows * top, most, lean, False)
    places = jnp.arange(number_of)

    def named(sizes, turn):
        used = int((sizes > 0).sum())
        fixed = max(1, used // 4)
        moved = fixed + (places - fixed + turn * (used - fixed)) % max(1, number_of - fixed)
        return jnp.zeros((number_of,), jnp.int32).at[order[jnp.where(places < fixed, places, moved)]].set(jnp.asarray(sizes, jnp.int32))

    sizes = jnp.where(number % 4 == 0, named(crowded, number // 4), named(ordinary, number - number // 4 - 1))
    mixed = jax.random.permutation(jax.random.fold_in(own, 3), number_of)
    donor, receiver = mixed[0:number_of // 2 * 2:2], mixed[1:number_of // 2 * 2:2]
    margin = jnp.minimum(sizes[donor] - 1, most - sizes[receiver]) // 2
    margin = jnp.where((donor == order[0]) | (receiver == order[0]) | (sizes[receiver] == 0), 0, jnp.maximum(margin, 0))
    moved = jax.random.randint(jax.random.fold_in(own, 4), (number_of // 2,), 0, 1 << 20) % (margin + 1)
    sizes = sizes.at[donor].add(-moved).at[receiver].add(moved)
    items = jnp.searchsorted(jnp.cumsum(sizes), jnp.arange(rows * top), side="right").astype(jnp.int32)
    table = items.reshape(top, rows).T
    table = table[jax.random.permutation(jax.random.fold_in(own, 1), rows)]
    turn = jax.random.randint(jax.random.fold_in(own, 2), (rows, 1), 0, top)
    return jnp.take_along_axis(table, (jnp.arange(top)[None, :] + turn) % top, axis=1)


def portions_of(number_of, total, bound, lean, full):
    portions = [(1 << 20) // math.isqrt(grade ** lean) + 1 for grade in range(1, number_of + 1)]
    largest = bound if full else min(bound, max(-(-total // number_of), total * portions[0] // sum(portions)))
    least = 1 if total - largest >= number_of - 1 else 0
    given, spare = [largest] + [least] * (number_of - 1), total - largest - least * (number_of - 1)
    while spare > 0:
        free = [i for i in range(1, number_of) if given[i] < largest] or [i for i in range(1, number_of) if given[i] < bound]
        whole, remaining = sum([portions[i] for i in free]), spare
        for i in free:
            extra = min(bound - given[i], max(1, remaining * portions[i] // whole), spare)
            given[i] = given[i] + extra
            spare = spare - extra
    return np.array(given)


def scatter_about(stream_key, shape, scale, reach, cuts=(), held_as=jnp.bfloat16):
    array = jax.random.normal(stream_key, shape, jnp.float32) * scale
    if len(cuts) > 0:
        array = block_scale(stream_key, shape, cuts, -0.22, 0.18) * array
    return jnp.clip(array, min=-reach, max=reach).astype(held_as)


def setup_inputs(seed: int = 0, part: int = 0) -> dict:
    streams_of = jax.random.split(jax.random.key(seed), 19)
    own_keys = jax.random.split(jax.random.fold_in(streams_of[18], part), 19)
    tokens = scatter_about(own_keys[0], (SEQS, D), 1.0, 6.0, ((0, 16),))
    cache_latent = scatter_about(own_keys[1], (SEQS, CACHE, LATENT), 1.0, 6.0, ((0, 16),))
    cache_rope = draw_cache_rope(jax.random.fold_in(jax.random.fold_in(streams_of[18], part), 71), part)
    lengths = draw_lengths(jax.random.fold_in(jax.random.fold_in(streams_of[18], part), 71), part)
    w_query = scatter_about(streams_of[4], (D, HEADS * (NOPE + ROPE)), D ** -0.5, 0.125, ((0, 16),))
    w_latent = scatter_about(streams_of[5], (D, LATENT), D ** -0.5, 0.125, ((0, 16),))
    w_rope = scatter_about(streams_of[6], (D, ROPE), D ** -0.5, 0.125, ((0, 16),))
    w_absorb = scatter_about(streams_of[7], (LATENT, HEADS * NOPE), LATENT ** -0.5, 0.25)
    w_value = scatter_about(streams_of[8], (LATENT, HEADS * VDIM), LATENT ** -0.5, 0.25)
    w_output = scatter_about(streams_of[9], (HEADS * VDIM, D), (HEADS * VDIM) ** -0.5, 0.1875, ((0, 16),))
    gain_attn = jnp.clip(1.0 + 0.18 * jax.random.normal(streams_of[10], (D,), jnp.float32), 0.1, 1.9)
    gain_latent = jnp.clip(1.0 + 0.18 * jax.random.normal(streams_of[11], (LATENT,), jnp.float32), 0.1, 1.9)
    gain_moe = jnp.clip(1.0 + 0.18 * jax.random.normal(streams_of[12], (D,), jnp.float32), 0.1, 1.9)
    routes_keys = jax.random.split(jax.random.fold_in(own_keys[13], 1), SEQS // SEQS)
    routes_turns = jax.random.permutation(jax.random.fold_in(own_keys[13], 3), SEQS // SEQS)
    routes = jax.vmap(lambda own, number: assign_block(jax.random.fold_in(own_keys[13], 2), own, number, SEQS, EXPERTS, TOPK, CAP, 2))(routes_keys, routes_turns).reshape((SEQS, TOPK))
    route_scores = jnp.clip(jnp.exp(math.log(1.0) - 1.609438 * jax.random.uniform(own_keys[14], (SEQS, TOPK), jnp.float32) ** block_scale(own_keys[14], (SEQS, TOPK), ((0, 16),), -0.2, 0.2)), 0.2, 1.0)
    w_gate = scatter_about(streams_of[15], (EXPERTS, D, FF), D ** -0.5, 0.125, ((0, 16),))
    w_up = scatter_about(streams_of[16], (EXPERTS, D, FF), D ** -0.5, 0.125, ((0, 16),))
    w_down = scatter_about(streams_of[17], (EXPERTS, FF, D), FF ** -0.5, 0.25, ((0, 16),))
    return {"tokens": tokens, "cache_latent": cache_latent, "cache_rope": cache_rope, "lengths": lengths, "w_query": w_query, "w_latent": w_latent, "w_rope": w_rope, "w_absorb": w_absorb, "w_value": w_value, "w_output": w_output, "gain_attn": gain_attn, "gain_latent": gain_latent, "gain_moe": gain_moe, "routes": routes, "route_scores": route_scores, "w_gate": w_gate, "w_up": w_up, "w_down": w_down}


EPS = 1e-06
THETA = 10000.0

def rms_scale(values, gain):
    return values * lax.rsqrt(lax.optimization_barrier(jnp.mean(values * values, axis=-1, keepdims=True)) + EPS) * gain.astype(jnp.float32)

def rope_tables(positions, width):
    inverse = THETA ** (-jnp.arange(0, width, 2).astype(jnp.float32) / width)
    angle = positions.astype(jnp.float32)[:, None] * inverse[None, :]
    return (jnp.cos(angle), jnp.sin(angle))

def apply_rope(values, cosine, sine):
    half = values.shape[-1] // 2
    first, second = (values[..., :half], values[..., half:])
    return jnp.concatenate([first * cosine - second * sine, second * cosine + first * sine], axis=-1)

def attend_one(items):
    q_abs, q_pe, lat_cache, rope_cache, ckv, kpe, length = items
    scale = (NOPE + ROPE) ** (-0.5)
    past = (jnp.einsum('hc,kc->hk', q_abs.astype(jnp.float32), lat_cache.astype(jnp.float32)) + jnp.einsum('hr,rk->hk', q_pe.astype(jnp.float32), rope_cache.astype(jnp.float32))) * scale
    fresh = (jnp.einsum('hc,c->h', q_abs.astype(jnp.float32), ckv.astype(jnp.float32)) + jnp.einsum('hr,r->h', q_pe.astype(jnp.float32), kpe.astype(jnp.float32))) * scale
    valid = jnp.arange(lat_cache.shape[0]).astype(jnp.int32)[None, :] < length
    top = jnp.maximum(lax.optimization_barrier(jnp.max(jnp.where(valid, past, -jnp.inf), axis=-1)), fresh)
    e_past = jnp.where(valid, jnp.exp(past - top[:, None]), 0.0)
    e_new = jnp.exp(fresh - top)
    total = lax.optimization_barrier(jnp.sum(e_past, axis=-1)) + e_new
    p_past = (e_past / total[:, None]).astype(jnp.bfloat16)
    p_new = (e_new / total).astype(jnp.bfloat16)
    out = jnp.einsum('hk,kc->hc', p_past.astype(jnp.float32), lat_cache.astype(jnp.float32)) + p_new.astype(jnp.float32)[:, None] * ckv.astype(jnp.float32)[None, :]
    return out.astype(jnp.bfloat16)

def reference(tokens, cache_latent, cache_rope, lengths, w_query, w_latent, w_rope, w_absorb, w_value, w_output, gain_attn, gain_latent, gain_moe, routes, route_scores, w_gate, w_up, w_down):
    count = tokens.shape[0]
    normed = rms_scale(tokens.astype(jnp.float32), gain_attn).astype(jnp.bfloat16)
    query = jnp.dot(normed, w_query, preferred_element_type=jnp.float32).astype(jnp.bfloat16)
    latent_raw = jnp.dot(normed, w_latent, preferred_element_type=jnp.float32).astype(jnp.bfloat16)
    rope_raw = jnp.dot(normed, w_rope, preferred_element_type=jnp.float32).astype(jnp.bfloat16)
    new_latent = rms_scale(latent_raw.astype(jnp.float32), gain_latent).astype(jnp.bfloat16)
    cosine, sine = rope_tables(lengths, ROPE)
    new_rope = apply_rope(rope_raw.astype(jnp.float32), cosine, sine).astype(jnp.bfloat16)
    heads_view = query.reshape(count, HEADS, NOPE + ROPE)
    q_nope = heads_view[:, :, :NOPE]
    q_pe = apply_rope(heads_view[:, :, NOPE:].astype(jnp.float32), cosine[:, None, :], sine[:, None, :]).astype(jnp.bfloat16)
    q_abs = jnp.einsum('shn,chn->shc', q_nope.astype(jnp.float32), w_absorb.reshape(LATENT, HEADS, NOPE).astype(jnp.float32)).astype(jnp.bfloat16)
    attended = lax.map(attend_one, (q_abs, q_pe, cache_latent, cache_rope, new_latent, new_rope, lengths))
    values = jnp.einsum('shc,chv->shv', attended.astype(jnp.float32), w_value.reshape(LATENT, HEADS, VDIM).astype(jnp.float32)).astype(jnp.bfloat16)
    attn_out = jnp.dot(values.reshape(count, HEADS * VDIM), w_output, preferred_element_type=jnp.float32)
    resid = (tokens.astype(jnp.float32) + attn_out).astype(jnp.bfloat16)
    moe_in = rms_scale(resid.astype(jnp.float32), gain_moe).astype(jnp.bfloat16)

    def expert_one(items):
        index, row = items
        gate = jnp.dot(row[None, :], w_gate[index], preferred_element_type=jnp.float32)
        upper = jnp.dot(row[None, :], w_up[index], preferred_element_type=jnp.float32)
        hidden = (jax.nn.silu(gate) * upper).astype(jnp.bfloat16)
        return jnp.dot(hidden, w_down[index], preferred_element_type=jnp.float32).astype(jnp.bfloat16)[0]
    flat_ids = routes.reshape(-1).astype(jnp.int32)
    flat_rows = jnp.repeat(moe_in, TOPK, axis=0)
    expert_out = lax.map(expert_one, (flat_ids, flat_rows)).reshape(count, TOPK, D)
    route_weight = route_scores / lax.optimization_barrier(jnp.sum(route_scores, axis=-1, keepdims=True))
    moe_sum = lax.optimization_barrier(jnp.sum(route_weight[:, :, None] * expert_out.astype(jnp.float32), axis=1))
    mixed = (resid.astype(jnp.float32) + moe_sum).astype(jnp.bfloat16)
    return (mixed, new_latent, new_rope)
```

```python
import jax
import jax.numpy as jnp
from jax import lax
from jax.sharding import PartitionSpec as P

D = 2048
HEADS = 16
NOPE = 64
ROPE = 32
VDIM = 64
LATENT = 512
CAP = 4
LANES = 128


EPS = 1e-06
THETA = 10000.0


def rms_scale(values, gain):
    return values * lax.rsqrt(jnp.mean(values * values, axis=-1, keepdims=True) + EPS) * gain


def rope_tables(positions, width):
    inverse = THETA ** (-jnp.arange(0, width, 2).astype(jnp.float32) / width)
    angle = positions.astype(jnp.float32)[:, None] * inverse[None, :]
    return (jnp.cos(angle), jnp.sin(angle))


def apply_rope(values, cosine, sine):
    half = values.shape[-1] // 2
    first, second = (values[..., :half], values[..., half:])
    return jnp.concatenate(
        [first * cosine - second * sine, second * cosine + first * sine], axis=-1
    )


def body(
    tokens,
    cache_latent,
    cache_rope,
    lengths,
    w_query,
    w_latent,
    w_rope,
    w_absorb,
    w_value,
    w_output,
    gain_attn,
    gain_latent,
    gain_moe,
    routes,
    route_scores,
    w_gate,
    w_up,
    w_down,
):
    local_seqs, width = tokens.shape
    devices = lax.axis_size("ep")
    me = lax.axis_index("ep")
    total_rows = devices * local_seqs
    block = w_query.shape[0]
    heads = HEADS
    q_width = w_query.shape[1]
    lat_width = w_latent.shape[1]
    bf16, f32 = jnp.bfloat16, jnp.float32

    top_k = routes.shape[1]
    tagged = jnp.concatenate(
        [tokens, routes.astype(bf16), jnp.zeros((local_seqs, LANES - top_k), bf16)], axis=1
    )
    tagged = jnp.broadcast_to(tagged[None], (devices,) + tagged.shape).reshape(total_rows, -1)
    gathered = lax.all_to_all(tagged, "ep", split_axis=0, concat_axis=0, tiled=True)
    all_tokens = gathered[:, :width]
    all_routes = gathered[:, width : width + top_k].astype(jnp.int32)

    all32 = all_tokens.astype(f32)
    scale_rows = lax.rsqrt(jnp.mean(all32 * all32, axis=-1, keepdims=True) + EPS)
    my_cols = lax.dynamic_slice_in_dim(all_tokens, me * block, block, axis=1).astype(f32)
    my_gain = lax.dynamic_slice_in_dim(gain_attn, me * block, block, axis=0)
    rows = (my_cols * scale_rows * my_gain).astype(bf16)
    partial = jnp.concatenate(
        [
            jnp.dot(rows, w_query, preferred_element_type=f32),
            jnp.dot(rows, w_latent, preferred_element_type=f32),
            jnp.dot(rows, w_rope, preferred_element_type=f32),
        ],
        axis=1,
    )
    partial = lax.all_to_all(partial, "ep", split_axis=0, concat_axis=0, tiled=True)
    summed = jnp.sum(partial.reshape(devices, local_seqs, -1), axis=0)

    token_ids = jnp.arange(total_rows)
    expert_ids = jnp.arange(devices)
    chosen = jnp.any(all_routes[:, :, None] == expert_ids[None, None, :], axis=1)
    before = (token_ids[None, :] < token_ids[:, None]).astype(bf16)
    rank = jnp.dot(before, chosen.astype(bf16), preferred_element_type=f32)
    ranked = jnp.where(chosen, rank, -1.0)
    slots = jnp.arange(CAP).astype(f32)
    routed = ranked.T[:, None, :] == slots[None, :, None]
    owned = (
        token_ids[None, None, :]
        == (expert_ids[:, None] * local_seqs + jnp.arange(local_seqs)[None, :])[:, :, None]
    )
    sel = jnp.concatenate([owned, routed], axis=1).astype(bf16)
    per = local_seqs + CAP
    sel_mine = lax.dynamic_slice_in_dim(sel, me, 1, axis=0)[0]
    tokens_mine = jnp.dot(sel_mine, all_tokens, preferred_element_type=f32)
    picker = sel_mine[local_seqs:]
    hits = routes[:, :, None] == expert_ids[None, None, :]
    route_weight = route_scores / jnp.sum(route_scores, axis=-1, keepdims=True)
    weight_table = jnp.sum(hits.astype(f32) * route_weight[:, :, None], axis=1)

    query = summed[:, :q_width].astype(bf16)
    latent_raw = summed[:, q_width : q_width + lat_width].astype(bf16)
    rope_raw = summed[:, q_width + lat_width :].astype(bf16)
    new_latent = rms_scale(latent_raw.astype(f32), gain_latent).astype(bf16)
    cosine, sine = rope_tables(lengths, ROPE)
    new_rope = apply_rope(rope_raw.astype(f32), cosine, sine).astype(bf16)
    heads_view = query.reshape(local_seqs, heads, NOPE + ROPE)
    q_nope = heads_view[:, :, :NOPE]
    q_pe = apply_rope(
        heads_view[:, :, NOPE:].astype(f32), cosine[:, None, :], sine[:, None, :]
    ).astype(bf16)
    head_ids = jnp.arange(heads)
    own_key = (jnp.arange(heads * NOPE) // NOPE)[None, None, :] == head_ids[None, :, None]
    spread_q = jnp.where(own_key, jnp.tile(q_nope, (1, 1, heads)), jnp.zeros((), bf16))
    q_abs = jnp.einsum("shm,cm->shc", spread_q, w_absorb, preferred_element_type=f32).astype(bf16)
    scale = (NOPE + ROPE) ** (-0.5)
    past = (
        jnp.einsum("shc,skc->shk", q_abs, cache_latent, preferred_element_type=f32)
        + jnp.einsum("shr,srk->shk", q_pe, cache_rope, preferred_element_type=f32)
    ) * scale
    fresh = (
        jnp.einsum("shc,sc->sh", q_abs, new_latent, preferred_element_type=f32)
        + jnp.einsum("shr,sr->sh", q_pe, new_rope, preferred_element_type=f32)
    ) * scale
    valid = jnp.arange(cache_latent.shape[1])[None, None, :] < lengths[:, None, None]
    top = jnp.maximum(jnp.max(jnp.where(valid, past, -jnp.inf), axis=-1), fresh)
    e_past = jnp.where(valid, jnp.exp(past - top[:, :, None]), 0.0)
    e_new = jnp.exp(fresh - top)
    total = jnp.sum(e_past, axis=-1) + e_new
    p_past = (e_past / total[:, :, None]).astype(bf16)
    p_new = (e_new / total).astype(bf16)
    attended = (
        jnp.einsum("shk,skc->shc", p_past, cache_latent, preferred_element_type=f32)
        + p_new.astype(f32)[:, :, None] * new_latent.astype(f32)[:, None, :]
    ).astype(bf16)
    all_heads = jnp.einsum("shc,cm->shm", attended, w_value, preferred_element_type=f32)
    own_value = (jnp.arange(heads * VDIM) // VDIM)[None, None, :] == head_ids[None, :, None]
    values = jnp.sum(jnp.where(own_value, all_heads, 0.0), axis=1).astype(bf16)

    head_rows = lax.all_to_all(values, "ep", split_axis=1, concat_axis=0, tiled=True)
    picked = jnp.dot(sel.reshape(devices * per, total_rows), head_rows,
                     preferred_element_type=f32).astype(bf16)
    out_part = jnp.dot(picked, w_output, preferred_element_type=f32).astype(bf16)
    out_part = lax.all_to_all(
        out_part.reshape(devices, per, width), "ep", split_axis=0, concat_axis=0, tiled=True
    )
    attn_out = jnp.sum(out_part.astype(f32), axis=0)
    resid = (tokens_mine + attn_out).astype(bf16)
    moe_in = rms_scale(resid.astype(f32), gain_moe).astype(bf16)
    packed = moe_in[local_seqs:]
    gate = jnp.dot(packed, w_gate[0], preferred_element_type=f32)
    upper = jnp.dot(packed, w_up[0], preferred_element_type=f32)
    hidden = (jax.nn.silu(gate) * upper).astype(bf16)
    result = jnp.dot(hidden, w_down[0], preferred_element_type=f32).astype(bf16)
    spread = jnp.dot(picker.T, result, preferred_element_type=f32).astype(bf16)
    answers = lax.all_to_all(spread, "ep", split_axis=0, concat_axis=0, tiled=True)
    answers = answers.reshape(devices, local_seqs, width)
    moe_sum = jnp.einsum("sn,nsd->sd", weight_table, answers.astype(f32))
    mixed = (resid[:local_seqs].astype(f32) + moe_sum).astype(bf16)
    return (mixed, new_latent, new_rope)


def solution(mesh):
    placed = (
        P(("grp", "ep"), None),
        P(("grp", "ep"), None, None),
        P(("grp", "ep"), None, None),
        P(("grp", "ep")),
        P("ep", None),
        P("ep", None),
        P("ep", None),
        P(),
        P(),
        P("ep", None),
        P(),
        P(),
        P(),
        P(("grp", "ep"), None),
        P(("grp", "ep"), None),
        P("ep", None, None),
        P("ep", None, None),
        P("ep", None, None),
    )
    return jax.shard_map(
        body,
        mesh=mesh,
        in_specs=placed,
        out_specs=(P(("grp", "ep"), None), P(("grp", "ep"), None), P(("grp", "ep"), None)),
        check_vma=False,
    )
```

```python
import jax
import jax.numpy as jnp
from jax import lax
from jax.experimental import pallas as pl
from jax.experimental.pallas import tpu as pltpu
from jax.sharding import PartitionSpec as P

D = 2048
HEADS = 16
NOPE = 64
ROPE = 32
VDIM = 64
LATENT = 512
CAP = 4
LANES = 128


EPS = 1e-06
THETA = 10000.0


def rms_scale(values, gain):
    return values * lax.rsqrt(jnp.mean(values * values, axis=-1, keepdims=True) + EPS) * gain


def rope_tables(positions, width):
    inverse = THETA ** (-jnp.arange(0, width, 2).astype(jnp.float32) / width)
    angle = positions.astype(jnp.float32)[:, None] * inverse[None, :]
    return (jnp.cos(angle), jnp.sin(angle))


def apply_rope(values, cosine, sine):
    half = values.shape[-1] // 2
    first, second = (values[..., :half], values[..., half:])
    return jnp.concatenate(
        [first * cosine - second * sine, second * cosine + first * sine], axis=-1
    )


def project_kernel(tokens_ref, cols_ref, gain_ref, wq_ref, wl_ref, wr_ref, tag_ref, out_ref):
    f32 = jnp.float32
    wide = tokens_ref[...].astype(f32)
    scale = lax.rsqrt(jnp.mean(wide * wide, axis=-1, keepdims=True) + EPS)
    rows = (cols_ref[...].astype(f32) * scale * gain_ref[...]).astype(jnp.bfloat16)
    q = jnp.dot(rows, wq_ref[...], preferred_element_type=f32)
    lat = jnp.dot(rows, wl_ref[...], preferred_element_type=f32)
    last = jnp.dot(rows, wr_ref[...], preferred_element_type=f32) + tag_ref[...]
    qw, lw = q.shape[1], lat.shape[1]
    for i in range(rows.shape[0]):
        out_ref[i, :, 0:qw] = q[i : i + 1]
        out_ref[i, :, qw : qw + lw] = lat[i : i + 1]
        out_ref[i, :, qw + lw :] = last[i : i + 1]


def expert_kernel(
    parts_ref, tok_ref, gain_ref, pick_ref, wg_hbm, wu_hbm, wd_hbm,
    resid_ref, out_ref, x_ref, wg, wu, wd, sems,
):
    f32, bf16 = jnp.float32, jnp.bfloat16
    loads = [
        pltpu.make_async_copy(src.at[0], dst, sems.at[n])
        for n, (src, dst) in enumerate(((wg_hbm, wg), (wu_hbm, wu), (wd_hbm, wd)))
    ]
    for load in loads:
        load.start()
    half = parts_ref.shape[-1]
    for k in range(parts_ref.shape[1]):
        part = jnp.sum(parts_ref[:, k].astype(f32), axis=0)
        x_ref[k : k + 1, 0:half] = part[0:1]
        x_ref[k : k + 1, half:] = part[1:2]
    resid = (tok_ref[...] + x_ref[...]).astype(bf16)
    wide = resid.astype(f32)
    scale = lax.rsqrt(jnp.mean(wide * wide, axis=-1, keepdims=True) + EPS)
    rows = (wide * scale * gain_ref[...]).astype(bf16)
    resid_ref[...] = resid[0 : resid_ref.shape[0]]
    loads[0].wait()
    gate = jnp.dot(rows, wg[...], preferred_element_type=f32)
    loads[1].wait()
    upper = jnp.dot(rows, wu[...], preferred_element_type=f32)
    hidden = (gate * jax.nn.sigmoid(gate) * upper).astype(bf16)
    loads[2].wait()
    result = jnp.dot(hidden, wd[...], preferred_element_type=f32).astype(bf16)
    spread = jnp.dot(pick_ref[...], result, preferred_element_type=f32)
    for i in range(spread.shape[0]):
        out_ref[i, 0:1, :] = spread[i : i + 1, 0:half].astype(bf16)
        out_ref[i, 1:2, :] = spread[i : i + 1, half:].astype(bf16)


def body(
    tokens,
    cache_latent,
    cache_rope,
    lengths,
    w_query,
    w_latent,
    w_rope,
    w_absorb,
    w_value,
    w_output,
    gain_attn,
    gain_latent,
    gain_moe,
    routes,
    route_scores,
    w_gate,
    w_up,
    w_down,
):
    local_seqs, width = tokens.shape
    devices = lax.axis_size("ep")
    me = lax.axis_index("ep")
    total_rows = devices * local_seqs
    block = w_query.shape[0]
    heads = HEADS
    q_width = w_query.shape[1]
    lat_width = w_latent.shape[1]
    bf16, f32 = jnp.bfloat16, jnp.float32

    top_k = routes.shape[1]
    half = width // 2
    copies = jnp.broadcast_to(
        tokens.reshape(1, local_seqs, 2, half), (devices, local_seqs, 2, half)
    ).reshape(total_rows, 2, half)
    gathered = lax.all_to_all(copies, "ep", split_axis=0, concat_axis=0, tiled=True)
    all_tokens = gathered.reshape(total_rows, width)
    my_cols = lax.dynamic_slice_in_dim(all_tokens, me * block, block, axis=1)
    my_gain = lax.dynamic_slice_in_dim(gain_attn, me * block, block, axis=0)[None]
    pe_width = w_rope.shape[1]
    last = pe_width + local_seqs * top_k
    last += -last % LANES
    w_last = jnp.pad(w_rope, ((0, 0), (0, last - pe_width)))
    tag = jnp.pad(
        routes.reshape(1, -1).astype(f32),
        ((0, 0), (pe_width, last - pe_width - local_seqs * top_k)),
    )
    sum_width = q_width + lat_width + pe_width
    partial = pl.pallas_call(
        project_kernel,
        out_shape=jax.ShapeDtypeStruct((total_rows, 1, q_width + lat_width + last), f32),
        name="project",
    )(all_tokens, my_cols, my_gain, w_query, w_latent, w_last, tag)
    partial = lax.all_to_all(partial, "ep", split_axis=0, concat_axis=0, tiled=True)
    partial = partial.reshape(devices, local_seqs, -1)
    summed = jnp.sum(partial[:, :, :sum_width], axis=0)
    all_routes = partial[:, 0, sum_width : sum_width + local_seqs * top_k]
    all_routes = all_routes.reshape(total_rows, top_k).astype(jnp.int32)

    token_ids = jnp.arange(total_rows)
    expert_ids = jnp.arange(devices)
    chosen = jnp.any(all_routes[:, :, None] == expert_ids[None, None, :], axis=1)
    before = (token_ids[None, :] < token_ids[:, None]).astype(bf16)
    rank = jnp.dot(before, chosen.astype(bf16), preferred_element_type=f32)
    ranked = jnp.where(chosen, rank, -1.0)
    slots = jnp.arange(CAP).astype(f32)
    routed = ranked.T[:, None, :] == slots[None, :, None]
    owned = (
        token_ids[None, None, :]
        == (expert_ids[:, None] * local_seqs + jnp.arange(local_seqs)[None, :])[:, :, None]
    )
    sel = jnp.concatenate([owned, routed], axis=1).astype(bf16)
    per = local_seqs + CAP
    sel_mine = lax.dynamic_slice_in_dim(sel, me, 1, axis=0)[0]
    tokens_mine = jnp.dot(sel_mine, all_tokens, preferred_element_type=f32)
    pick = jnp.where(jnp.arange(per)[None, :] >= local_seqs, sel_mine.T, jnp.zeros((), bf16))
    hits = routes[:, :, None] == expert_ids[None, None, :]
    route_weight = route_scores / jnp.sum(route_scores, axis=-1, keepdims=True)
    weight_table = jnp.sum(hits.astype(f32) * route_weight[:, :, None], axis=1)

    query = summed[:, :q_width].astype(bf16)
    latent_raw = summed[:, q_width : q_width + lat_width].astype(bf16)
    rope_raw = summed[:, q_width + lat_width :].astype(bf16)
    new_latent = rms_scale(latent_raw.astype(f32), gain_latent).astype(bf16)
    cosine, sine = rope_tables(lengths, ROPE)
    new_rope = apply_rope(rope_raw.astype(f32), cosine, sine).astype(bf16)
    heads_view = query.reshape(local_seqs, heads, NOPE + ROPE)
    q_nope = heads_view[:, :, :NOPE]
    q_pe = apply_rope(
        heads_view[:, :, NOPE:].astype(f32), cosine[:, None, :], sine[:, None, :]
    ).astype(bf16)
    head_ids = jnp.arange(heads)
    own_key = (jnp.arange(heads * NOPE) // NOPE)[None, None, :] == head_ids[None, :, None]
    spread_q = jnp.where(own_key, jnp.tile(q_nope, (1, 1, heads)), jnp.zeros((), bf16))
    q_abs = jnp.einsum("shm,cm->shc", spread_q, w_absorb, preferred_element_type=f32).astype(bf16)
    scale = (NOPE + ROPE) ** (-0.5)
    past = (
        jnp.einsum("shc,skc->shk", q_abs, cache_latent, preferred_element_type=f32)
        + jnp.einsum("shr,srk->shk", q_pe, cache_rope, preferred_element_type=f32)
    ) * scale
    fresh = (
        jnp.einsum("shc,sc->sh", q_abs, new_latent, preferred_element_type=f32)
        + jnp.einsum("shr,sr->sh", q_pe, new_rope, preferred_element_type=f32)
    ) * scale
    valid = jnp.arange(cache_latent.shape[1])[None, None, :] < lengths[:, None, None]
    top = jnp.maximum(jnp.max(jnp.where(valid, past, -jnp.inf), axis=-1), fresh)
    e_past = jnp.where(valid, jnp.exp(past - top[:, :, None]), 0.0)
    e_new = jnp.exp(fresh - top)
    total = jnp.sum(e_past, axis=-1) + e_new
    p_past = (e_past / total[:, :, None]).astype(bf16)
    p_new = (e_new / total).astype(bf16)
    attended = (
        jnp.einsum("shk,skc->shc", p_past, cache_latent, preferred_element_type=f32)
        + p_new.astype(f32)[:, :, None] * new_latent.astype(f32)[:, None, :]
    ).astype(bf16)
    all_heads = jnp.einsum("shc,cm->shm", attended, w_value, preferred_element_type=f32)
    own_value = (jnp.arange(heads * VDIM) // VDIM)[None, None, :] == head_ids[None, :, None]
    values = jnp.sum(jnp.where(own_value, all_heads, 0.0), axis=1).astype(bf16)

    head_rows = lax.all_to_all(values, "ep", split_axis=1, concat_axis=0, tiled=True)
    picked = jnp.dot(sel.reshape(devices * per, total_rows), head_rows,
                     preferred_element_type=f32).astype(bf16)
    out_part = jnp.dot(picked, w_output, preferred_element_type=f32).astype(bf16)
    out_part = lax.all_to_all(
        out_part.reshape(devices, per, 2, half), "ep", split_axis=0, concat_axis=0, tiled=True
    )
    ff = w_gate.shape[2]
    whole = pl.BlockSpec(memory_space=pltpu.VMEM)
    far = pl.BlockSpec(memory_space=pl.ANY)
    resid, spread = pl.pallas_call(
        expert_kernel,
        out_shape=(
            jax.ShapeDtypeStruct((local_seqs, width), bf16),
            jax.ShapeDtypeStruct((total_rows, 2, half), bf16),
        ),
        in_specs=[whole] * 4 + [far] * 3,
        out_specs=(whole, whole),
        scratch_shapes=[
            pltpu.VMEM((per, width), f32),
            pltpu.VMEM((width, ff), bf16),
            pltpu.VMEM((width, ff), bf16),
            pltpu.VMEM((ff, width), bf16),
            pltpu.SemaphoreType.DMA((3,)),
        ],
        name="experts",
    )(out_part, tokens_mine, gain_moe[None], pick, w_gate, w_up, w_down)
    answers = lax.all_to_all(spread, "ep", split_axis=0, concat_axis=0, tiled=True)
    answers = answers.reshape(devices, local_seqs, width)
    moe_sum = jnp.einsum("sn,nsd->sd", weight_table, answers.astype(f32))
    mixed = (resid.astype(f32) + moe_sum).astype(bf16)
    return (mixed, new_latent, new_rope)


def solution(mesh):
    placed = (
        P(("grp", "ep"), None),
        P(("grp", "ep"), None, None),
        P(("grp", "ep"), None, None),
        P(("grp", "ep")),
        P("ep", None),
        P("ep", None),
        P("ep", None),
        P(),
        P(),
        P("ep", None),
        P(),
        P(),
        P(),
        P(("grp", "ep"), None),
        P(("grp", "ep"), None),
        P("ep", None, None),
        P("ep", None, None),
        P("ep", None, None),
    )
    return jax.shard_map(
        body,
        mesh=mesh,
        in_specs=placed,
        out_specs=(P(("grp", "ep"), None), P(("grp", "ep"), None), P(("grp", "ep"), None)),
        check_vma=False,
    )
```

```python
import jax
import jax.numpy as jnp
from jax import lax
from jax.experimental import pallas as pl
from jax.experimental.pallas import tpu as pltpu
from jax.sharding import PartitionSpec as P

D = 2048
HEADS = 16
NOPE = 64
ROPE = 32
VDIM = 64
LATENT = 512
CAP = 4
LANES = 128


EPS = 1e-06
THETA = 10000.0


def rms_scale(values, gain):
    return values * lax.rsqrt(jnp.mean(values * values, axis=-1, keepdims=True) + EPS) * gain


def rope_tables(positions, width):
    inverse = THETA ** (-jnp.arange(0, width, 2).astype(jnp.float32) / width)
    angle = positions.astype(jnp.float32)[:, None] * inverse[None, :]
    return (jnp.cos(angle), jnp.sin(angle))


def apply_rope(values, cosine, sine):
    half = values.shape[-1] // 2
    first, second = (values[..., :half], values[..., half:])
    return jnp.concatenate(
        [first * cosine - second * sine, second * cosine + first * sine], axis=-1
    )


def project_kernel(tokens_ref, cols_ref, gain_ref, wq_ref, wl_ref, wr_ref, tag_ref, out_ref):
    f32 = jnp.float32
    wide = tokens_ref[...].astype(f32)
    scale = lax.rsqrt(jnp.mean(wide * wide, axis=-1, keepdims=True) + EPS)
    rows = (cols_ref[...].astype(f32) * scale * gain_ref[...]).astype(jnp.bfloat16)
    q = jnp.dot(rows, wq_ref[...], preferred_element_type=f32)
    lat = jnp.dot(rows, wl_ref[...], preferred_element_type=f32)
    last = jnp.dot(rows, wr_ref[...], preferred_element_type=f32) + tag_ref[...]
    qw, lw = q.shape[1], lat.shape[1]
    for i in range(rows.shape[0]):
        out_ref[i, :, 0:qw] = q[i : i + 1]
        out_ref[i, :, qw : qw + lw] = lat[i : i + 1]
        out_ref[i, :, qw + lw :] = last[i : i + 1]


def expert_kernel(
    parts_ref, tok_ref, gain_ref, pick_ref, wg_hbm, wu_hbm, wd_hbm,
    resid_ref, out_ref, x_ref, wg, wu, wd, sems,
):
    f32, bf16 = jnp.float32, jnp.bfloat16
    loads = [
        pltpu.make_async_copy(src.at[0], dst, sems.at[n])
        for n, (src, dst) in enumerate(((wg_hbm, wg), (wu_hbm, wu), (wd_hbm, wd)))
    ]
    for load in loads:
        load.start()
    half = parts_ref.shape[-1]
    for k in range(parts_ref.shape[1]):
        part = jnp.sum(parts_ref[:, k].astype(f32), axis=0)
        x_ref[k : k + 1, 0:half] = part[0:1]
        x_ref[k : k + 1, half:] = part[1:2]
    resid = (tok_ref[...] + x_ref[...]).astype(bf16)
    wide = resid.astype(f32)
    scale = lax.rsqrt(jnp.mean(wide * wide, axis=-1, keepdims=True) + EPS)
    rows = (wide * scale * gain_ref[...]).astype(bf16)
    resid_ref[...] = resid[0 : resid_ref.shape[0]]
    loads[0].wait()
    gate = jnp.dot(rows, wg[...], preferred_element_type=f32)
    loads[1].wait()
    upper = jnp.dot(rows, wu[...], preferred_element_type=f32)
    hidden = (gate * jax.nn.sigmoid(gate) * upper).astype(bf16)
    loads[2].wait()
    result = jnp.dot(hidden, wd[...], preferred_element_type=f32).astype(bf16)
    spread = jnp.dot(pick_ref[...], result, preferred_element_type=f32)
    for i in range(spread.shape[0]):
        out_ref[i, 0:1, :] = spread[i : i + 1, 0:half].astype(bf16)
        out_ref[i, 1:2, :] = spread[i : i + 1, half:].astype(bf16)


def attend_kernel(
    part_ref, gain_ref, cos_ref, sin_ref, len_ref, wa_hbm, wv_hbm, rope_hbm, lat_hbm,
    val_ref, newlat_ref, newrope_ref, q_ref, wa, wv, rope, lat, sems,
):
    f32, bf16 = jnp.float32, jnp.bfloat16
    seqs = newlat_ref.shape[0]
    devices = part_ref.shape[0] // seqs
    qw = HEADS * (NOPE + ROPE)
    lw = newlat_ref.shape[1]
    scale = (NOPE + ROPE) ** (-0.5)
    half = ROPE // 2
    load_wa = pltpu.make_async_copy(wa_hbm, wa, sems.at[0])
    load_wv = pltpu.make_async_copy(wv_hbm, wv, sems.at[1])
    load_wa.start()

    def turn(v, cosine, sine):
        first, second = v[:, :half], v[:, half:]
        return jnp.concatenate(
            [first * cosine - second * sine, second * cosine + first * sine], axis=1
        ).astype(bf16)

    def own_lanes(size, each):
        row = lax.broadcasted_iota(jnp.int32, (HEADS, size), 0)
        lane = lax.broadcasted_iota(jnp.int32, (HEADS, size), 1)
        return (lane >= row * each) & (lane < row * each + each)

    for s in range(seqs):
        load_rope = pltpu.make_async_copy(rope_hbm.at[s], rope, sems.at[2])
        load_lat = pltpu.make_async_copy(lat_hbm.at[s], lat, sems.at[3])
        load_rope.start()
        load_lat.start()
        if s == 0:
            load_wv.start()
        total = part_ref[s]
        for d in range(1, devices):
            total = total + part_ref[d * seqs + s]
        total = total.astype(bf16).astype(f32)
        cosine, sine = cos_ref[s : s + 1], sin_ref[s : s + 1]
        raw = total[:, qw : qw + lw]
        norm = lax.rsqrt(jnp.mean(raw * raw, axis=-1, keepdims=True) + EPS)
        new_latent = (raw * norm * gain_ref[...]).astype(bf16)
        new_rope = turn(total[:, qw + lw : qw + lw + ROPE], cosine, sine)
        newlat_ref[s : s + 1] = new_latent
        newrope_ref[s : s + 1] = new_rope
        each = NOPE + ROPE
        for h in range(HEADS):
            q_ref[h : h + 1, 0:each] = total[:, h * each : h * each + each]
        q = q_ref[:, 0:each]
        q_pe = turn(q[:, NOPE:], cosine, sine)
        spread = jnp.concatenate([q[:, :NOPE]] * HEADS, axis=1)
        spread = jnp.where(own_lanes(HEADS * NOPE, NOPE), spread, 0.0).astype(bf16)
        if s == 0:
            load_wa.wait()
        nt = (((1,), (1,)), ((), ()))
        q_abs = lax.dot_general(spread, wa[...], nt, preferred_element_type=f32).astype(bf16)
        fresh = (
            jnp.sum(q_abs.astype(f32) * new_latent.astype(f32), axis=1, keepdims=True)
            + jnp.sum(q_pe.astype(f32) * new_rope.astype(f32), axis=1, keepdims=True)
        ) * scale
        load_rope.wait()
        past = jnp.dot(q_pe, rope[...], preferred_element_type=f32)
        load_lat.wait()
        past = (past + lax.dot_general(q_abs, lat[...], nt, preferred_element_type=f32)) * scale
        valid = lax.broadcasted_iota(jnp.int32, past.shape, 1) < len_ref[s]
        top = jnp.max(jnp.where(valid, past, -jnp.inf), axis=1, keepdims=True)
        top = jnp.maximum(top, fresh)
        e_past = jnp.where(valid, jnp.exp(past - top), 0.0)
        e_new = jnp.exp(fresh - top)
        denom = jnp.sum(e_past, axis=1, keepdims=True) + e_new
        p_past = (e_past / denom).astype(bf16)
        p_new = (e_new / denom).astype(bf16).astype(f32)
        attended = (
            jnp.dot(p_past, lat[...], preferred_element_type=f32)
            + p_new * new_latent.astype(f32)
        ).astype(bf16)
        if s == 0:
            load_wv.wait()
        mixed = jnp.dot(attended, wv[...], preferred_element_type=f32)
        mixed = jnp.where(own_lanes(HEADS * VDIM, VDIM), mixed, 0.0)
        values = jnp.sum(mixed, axis=0, keepdims=True).astype(bf16)
        part = val_ref.shape[2]
        for d in range(devices):
            val_ref[d, s : s + 1, :] = values[:, d * part : d * part + part]


def body(
    tokens,
    cache_latent,
    cache_rope,
    lengths,
    w_query,
    w_latent,
    w_rope,
    w_absorb,
    w_value,
    w_output,
    gain_attn,
    gain_latent,
    gain_moe,
    routes,
    route_scores,
    w_gate,
    w_up,
    w_down,
):
    local_seqs, width = tokens.shape
    devices = lax.axis_size("ep")
    me = lax.axis_index("ep")
    total_rows = devices * local_seqs
    block = w_query.shape[0]
    heads = HEADS
    q_width = w_query.shape[1]
    lat_width = w_latent.shape[1]
    bf16, f32 = jnp.bfloat16, jnp.float32

    top_k = routes.shape[1]
    half = width // 2
    copies = jnp.broadcast_to(
        tokens.reshape(1, local_seqs, 2, half), (devices, local_seqs, 2, half)
    ).reshape(total_rows, 2, half)
    gathered = lax.all_to_all(copies, "ep", split_axis=0, concat_axis=0, tiled=True)
    all_tokens = gathered.reshape(total_rows, width)
    my_cols = lax.dynamic_slice_in_dim(all_tokens, me * block, block, axis=1)
    my_gain = lax.dynamic_slice_in_dim(gain_attn, me * block, block, axis=0)[None]
    pe_width = w_rope.shape[1]
    last = pe_width + local_seqs * top_k
    last += -last % LANES
    w_last = jnp.pad(w_rope, ((0, 0), (0, last - pe_width)))
    tag = jnp.pad(
        routes.reshape(1, -1).astype(f32),
        ((0, 0), (pe_width, last - pe_width - local_seqs * top_k)),
    )
    sum_width = q_width + lat_width + pe_width
    partial = pl.pallas_call(
        project_kernel,
        out_shape=jax.ShapeDtypeStruct((total_rows, 1, q_width + lat_width + last), f32),
        name="project",
    )(all_tokens, my_cols, my_gain, w_query, w_latent, w_last, tag)
    partial = lax.all_to_all(partial, "ep", split_axis=0, concat_axis=0, tiled=True)
    arrived = partial
    partial = partial.reshape(devices, local_seqs, -1)
    all_routes = partial[:, 0, sum_width : sum_width + local_seqs * top_k]
    all_routes = all_routes.reshape(total_rows, top_k).astype(jnp.int32)

    token_ids = jnp.arange(total_rows)
    expert_ids = jnp.arange(devices)
    chosen = jnp.any(all_routes[:, :, None] == expert_ids[None, None, :], axis=1)
    before = (token_ids[None, :] < token_ids[:, None]).astype(bf16)
    rank = jnp.dot(before, chosen.astype(bf16), preferred_element_type=f32)
    ranked = jnp.where(chosen, rank, -1.0)
    slots = jnp.arange(CAP).astype(f32)
    routed = ranked.T[:, None, :] == slots[None, :, None]
    owned = (
        token_ids[None, None, :]
        == (expert_ids[:, None] * local_seqs + jnp.arange(local_seqs)[None, :])[:, :, None]
    )
    sel = jnp.concatenate([owned, routed], axis=1).astype(bf16)
    per = local_seqs + CAP
    sel_mine = lax.dynamic_slice_in_dim(sel, me, 1, axis=0)[0]
    tokens_mine = jnp.dot(sel_mine, all_tokens, preferred_element_type=f32)
    pick = jnp.where(jnp.arange(per)[None, :] >= local_seqs, sel_mine.T, jnp.zeros((), bf16))
    hits = routes[:, :, None] == expert_ids[None, None, :]
    route_weight = route_scores / jnp.sum(route_scores, axis=-1, keepdims=True)
    weight_table = jnp.sum(hits.astype(f32) * route_weight[:, :, None], axis=1)

    cosine, sine = rope_tables(lengths, ROPE)
    whole = pl.BlockSpec(memory_space=pltpu.VMEM)
    far = pl.BlockSpec(memory_space=pl.ANY)
    slots_kept = cache_latent.shape[1]
    values, new_latent, new_rope = pl.pallas_call(
        attend_kernel,
        out_shape=(
            jax.ShapeDtypeStruct((devices, local_seqs, heads * VDIM // devices), bf16),
            jax.ShapeDtypeStruct((local_seqs, lat_width), bf16),
            jax.ShapeDtypeStruct((local_seqs, pe_width), bf16),
        ),
        in_specs=[whole] * 4 + [pl.BlockSpec(memory_space=pltpu.SMEM)] + [far] * 4,
        out_specs=(whole, whole, whole),
        scratch_shapes=[
            pltpu.VMEM((heads, LANES), f32),
            pltpu.VMEM(w_absorb.shape, bf16),
            pltpu.VMEM(w_value.shape, bf16),
            pltpu.VMEM((pe_width, slots_kept), bf16),
            pltpu.VMEM((slots_kept, lat_width), bf16),
            pltpu.SemaphoreType.DMA((4,)),
        ],
        name="attend",
    )(arrived, gain_latent[None], cosine, sine, lengths, w_absorb, w_value, cache_rope, cache_latent)

    head_rows = lax.all_to_all(values, "ep", split_axis=0, concat_axis=0, tiled=True)
    head_rows = head_rows.reshape(total_rows, -1)
    picked = jnp.dot(sel.reshape(devices * per, total_rows), head_rows,
                     preferred_element_type=f32).astype(bf16)
    out_part = jnp.dot(picked, w_output, preferred_element_type=f32).astype(bf16)
    out_part = lax.all_to_all(
        out_part.reshape(devices, per, 2, half), "ep", split_axis=0, concat_axis=0, tiled=True
    )
    ff = w_gate.shape[2]
    resid, spread = pl.pallas_call(
        expert_kernel,
        out_shape=(
            jax.ShapeDtypeStruct((local_seqs, width), bf16),
            jax.ShapeDtypeStruct((total_rows, 2, half), bf16),
        ),
        in_specs=[whole] * 4 + [far] * 3,
        out_specs=(whole, whole),
        scratch_shapes=[
            pltpu.VMEM((per, width), f32),
            pltpu.VMEM((width, ff), bf16),
            pltpu.VMEM((width, ff), bf16),
            pltpu.VMEM((ff, width), bf16),
            pltpu.SemaphoreType.DMA((3,)),
        ],
        name="experts",
    )(out_part, tokens_mine, gain_moe[None], pick, w_gate, w_up, w_down)
    answers = lax.all_to_all(spread, "ep", split_axis=0, concat_axis=0, tiled=True)
    answers = answers.reshape(devices, local_seqs, width)
    moe_sum = jnp.einsum("sn,nsd->sd", weight_table, answers.astype(f32))
    mixed = (resid.astype(f32) + moe_sum).astype(bf16)
    return (mixed, new_latent, new_rope)


def solution(mesh):
    placed = (
        P(("grp", "ep"), None),
        P(("grp", "ep"), None, None),
        P(("grp", "ep"), None, None),
        P(("grp", "ep")),
        P("ep", None),
        P("ep", None),
        P("ep", None),
        P(),
        P(),
        P("ep", None),
        P(),
        P(),
        P(),
        P(("grp", "ep"), None),
        P(("grp", "ep"), None),
        P("ep", None, None),
        P("ep", None, None),
        P("ep", None, None),
    )
    return jax.shard_map(
        body,
        mesh=mesh,
        in_specs=placed,
        out_specs=(P(("grp", "ep"), None), P(("grp", "ep"), None), P(("grp", "ep"), None)),
        check_vma=False,
    )
```
